32 devices in a mesh: sp: 8 (over z, y), tp: 4 (over x, core).
Axes of the slice: x: 2, y: 2, z: 4, core: 2. Of those that a mesh axis runs over, the one named last changes fastest.
Arguments:
- tokens: bfloat16 [6, 2048, 2048], P(None, 'sp', 'tp'), may hold values from -6 to 6
- norm_gains: float32 [3, 2048], replicated, may hold values from 0.5 to 1.5
- weight_outer: bfloat16 [3, 2048, 1024], P(None, 'sp', 'tp'), may hold values from -0.125 to 0.125
- weight_inner: bfloat16 [3, 2048, 1024], P(None, 'sp', 'tp'), may hold values from -0.125 to 0.125
- weight_value: bfloat16 [3, 2048, 1024], P(None, 'sp', 'tp'), may hold values from -0.125 to 0.125
- conv_taps: bfloat16 [3, 3, 1024], P(None, None, 'tp'), may hold values from -3.5 to 3.5
- weight_output: bfloat16 [3, 1024, 2048], P(None, 'sp', 'tp'), may hold values from -0.1875 to 0.1875
Outputs:
- mixed_out: float32 [6, 2048, 2048], P(None, 'sp', 'tp')
The draws below stay inside these ranges and needn't reach their ends.
All inputs are finite; a program needn't handle non-finite values.
Results may differ from the reference program's by a relative error of at most 0.03.
Values may be sent and summed in bfloat16 or wider, within the bound.
A program may use at most 128 MiB of HBM per device.

```python
import jax
import jax.numpy as jnp
from jax import lax

D = 2048
SC = 1024
KERNEL = 3
LAYERS = 3
SEQS = 6
SEQ = 2048


def shard_levels(key, dims, cuts, smallest, top_value):
    factor_of, own = 1.0, jax.random.fold_in(key, 6)
    for position, shards_of in cuts:
        draws = jnp.exp(jax.random.uniform(jax.random.fold_in(own, position), (shards_of,), jnp.float32, smallest / len(cuts), top_value / len(cuts)))
        factor_of = factor_of * jnp.repeat(draws, dims[position] // shards_of).reshape([-1 if axis == position else 1 for axis in range(len(dims))])
    return factor_of


def centred(stream_key, shape, scale, bound, pieces=(), held_as=jnp.bfloat16):
    values = scale * jax.random.normal(stream_key, shape, jnp.float32)
    if pieces:
        values = values * shard_levels(stream_key, shape, pieces, -0.22, 0.18)
    return jnp.clip(values, -bound, bound).astype(held_as)


def setup_inputs(seed: int = 0) -> dict:
    arg_keys = jax.random.split(jax.random.key(seed), 8)
    return {
        "tokens": centred(arg_keys[0], (SEQS, SEQ, D), 1.0, 6.0, ((1, 8), (2, 4))),
        "norm_gains": jnp.clip(1.0 + 0.1 * jax.random.normal(arg_keys[1], (LAYERS, D), jnp.float32), 0.5, 1.5),
        "weight_outer": centred(arg_keys[2], (LAYERS, D, SC), D ** -0.5, 0.125, ((1, 8), (2, 4))),
        "weight_inner": centred(arg_keys[3], (LAYERS, D, SC), D ** -0.5, 0.125, ((1, 8), (2, 4))),
        "weight_value": centred(arg_keys[4], (LAYERS, D, SC), D ** -0.5, 0.125, ((1, 8), (2, 4))),
        "conv_taps": centred(arg_keys[5], (LAYERS, KERNEL, SC), KERNEL ** -0.5, 3.5, ((2, 4),)),
        "weight_output": centred(arg_keys[6], (LAYERS, SC, D), SC ** -0.5, 0.1875, ((1, 8), (2, 4))),
    }


epsilon = 1e-06

def normalize(values_in, gain_row):
    values = values_in.astype(jnp.float32)
    scale = lax.rsqrt(lax.optimization_barrier(jnp.mean(values * values, axis=-1, keepdims=True)) + epsilon)
    return (values * scale * gain_row.astype(jnp.float32)).astype(jnp.bfloat16)

def reference(tokens, norm_gains, weight_outer, weight_inner, weight_value, conv_taps, weight_output):
    current = tokens
    projected = None
    for layer in range(LAYERS):
        normed = normalize(current, norm_gains[layer]).reshape(SEQS * SEQ, D)
        outer = jnp.dot(normed, weight_outer[layer], preferred_element_type=jnp.float32).astype(jnp.bfloat16)
        inner = jnp.dot(normed, weight_inner[layer], preferred_element_type=jnp.float32).astype(jnp.bfloat16)
        value = jnp.dot(normed, weight_value[layer], preferred_element_type=jnp.float32).astype(jnp.bfloat16)
        outer, inner, value = lax.optimization_barrier((outer, inner, value))
        gated = (inner.astype(jnp.float32) * value.astype(jnp.float32)).reshape(SEQS, SEQ, SC)
        padded = jnp.pad(gated, ((0, 0), (KERNEL - 1, 0), (0, 0)))
        conved = jnp.zeros((SEQS, SEQ, SC), jnp.float32)
        for offset in range(KERNEL):
            conved = conved + conv_taps[layer, offset].astype(jnp.float32) * padded[:, offset:offset + SEQ]
        mixer = (outer.astype(jnp.float32).reshape(SEQS, SEQ, SC) * conved).astype(jnp.bfloat16)
        projected = jnp.dot(mixer.reshape(SEQS * SEQ, SC), weight_output[layer], preferred_element_type=jnp.float32)
        current = projected.astype(jnp.bfloat16).reshape(SEQS, SEQ, D)
    return projected.reshape(SEQS, SEQ, D)
```

```python
import functools

import jax
import jax.numpy as jnp
from jax import lax
from jax.experimental import pallas as pl
from jax.experimental.pallas import tpu as pltpu
from jax.sharding import PartitionSpec as P

epsilon = 1e-06


def gather_kernel(plans, *refs):
    count = len(plans)
    shards, wholes, scratch = refs[:count], refs[count : 2 * count], refs[2 * count :]
    jobs = []
    for i, (axis, size, pair, dim) in enumerate(plans):
        me = lax.axis_index(axis)
        jobs.append((axis, size // pair, pair, dim, me // pair, me % pair, shards[i], wholes[i]) + tuple(scratch[6 * i : 6 * i + 6]))

    barrier = pltpu.get_barrier_semaphore()
    expected = jnp.int32(0)
    for axis, length, pair, _, spot, side, *_ in jobs:
        for step in (-1, 1):
            there = jnp.logical_and(spot + step >= 0, spot + step < length)
            expected = expected + there.astype(jnp.int32)

            @pl.when(there)
            def _(axis=axis, target=(spot + step) * pair + side):
                pl.semaphore_signal(barrier, inc=1, device_id={axis: target})

        if pair == 2:
            expected = expected + 1
            pl.semaphore_signal(barrier, inc=1, device_id={axis: spot * pair + 1 - side})
    pl.semaphore_wait(barrier, expected)

    def place(job, owner_spot, owner_side):
        pair, dim, shard, whole = job[2], job[3], job[6], job[7]
        extent = shard.shape[dim]
        start = pl.multiple_of((owner_spot * pair + owner_side) * extent, extent)
        return whole.at[pl.ds(start, extent), :] if dim == 0 else whole.at[:, pl.ds(start, extent)]

    def remote(job, kind, owner, own=False):
        axis, _, pair, _, spot, side, shard, _, line_recv, pair_recv, right, left, across, _ = job
        slot = place(job, owner, side)
        send, recv, target = {
            "right": (right, line_recv, (spot + 1) * pair + side),
            "left": (left, line_recv, (spot - 1) * pair + side),
            "across": (across, pair_recv, spot * pair + 1 - side),
        }[kind]
        return pltpu.make_async_remote_copy(
            src_ref=shard if own else slot,
            dst_ref=slot,
            send_sem=send.at[owner],
            recv_sem=recv.at[owner],
            device_id={axis: target},
        )

    def arrived(job, kind, owner):
        axis, _, pair, _, spot, side, _, _, line_recv, pair_recv, right, _, across, _ = job
        slot = place(job, owner, side if kind == "line" else 1 - side)
        recv = line_recv if kind == "line" else pair_recv
        pltpu.make_async_remote_copy(
            src_ref=slot,
            dst_ref=slot,
            send_sem=across.at[owner],
            recv_sem=recv.at[owner],
            device_id={axis: spot * pair + side},
        ).wait_recv()

    def spread(job, owner, go_right, go_left, own=False):
        spot, length, pair = job[4], job[1], job[2]
        if go_right:
            @pl.when(spot < length - 1)
            def _():
                remote(job, "right", owner, own).start()

        if go_left:
            @pl.when(spot > 0)
            def _():
                remote(job, "left", owner, own).start()

        if pair == 2:
            remote(job, "across", owner, own).start()

    for job in jobs:
        spread(job, job[4], True, True, own=True)
    for job in jobs:
        pltpu.make_async_copy(job[6], place(job, job[4], job[5]), job[13]).start()

    for job in jobs:
        spot, length = job[4], job[1]
        for distance in range(1, length):

            @pl.when(spot >= distance)
            def _(job=job, owner=spot - distance):
                arrived(job, "line", owner)
                spread(job, owner, True, False)

            @pl.when(spot + distance < length)
            def _(job=job, owner=spot + distance):
                arrived(job, "line", owner)
                spread(job, owner, False, True)

    for job in jobs:
        spot, length, pair = job[4], job[1], job[2]
        pltpu.make_async_copy(job[6], place(job, job[4], job[5]), job[13]).wait()
        for owner in range(length):
            if pair == 2:
                arrived(job, "across", owner)
                remote(job, "across", owner).wait_send()

            @pl.when(jnp.logical_and(spot >= owner, spot < length - 1))
            def _(job=job, owner=owner):
                remote(job, "right", owner).wait_send()

            @pl.when(jnp.logical_and(spot <= owner, spot > 0))
            def _(job=job, owner=owner):
                remote(job, "left", owner).wait_send()


def gather_all(parts, number):
    plans, shapes, scratch, sent = [], [], [], 0
    for array, axis, dim in parts:
        size = lax.axis_size(axis)
        pair = 2 if size % 2 == 0 else 1
        plans.append((axis, size, pair, dim))
        shape = list(array.shape)
        shape[dim] *= size
        shapes.append(jax.ShapeDtypeStruct(tuple(shape), array.dtype))
        sent += array.size * array.dtype.itemsize * size
        scratch += [pltpu.SemaphoreType.DMA((size // pair,))] * 5 + [pltpu.SemaphoreType.DMA]
    return pl.pallas_call(
        functools.partial(gather_kernel, tuple(plans)),
        out_shape=tuple(shapes),
        in_specs=[pl.BlockSpec(memory_space=pltpu.VMEM)] * len(parts),
        out_specs=tuple([pl.BlockSpec(memory_space=pl.ANY)] * len(parts)),
        scratch_shapes=scratch,
        cost_estimate=pl.CostEstimate(flops=0, bytes_accessed=10 * sent, transcendentals=0),
        compiler_params=pltpu.CompilerParams(collective_id=number, has_side_effects=True),
    )(*[array for array, _, _ in parts])


def from_behind(block, axis, distance):
    devices = range(lax.axis_size(axis))
    route = [(i - distance, i) for i in devices if i - distance in devices]
    return lax.ppermute(block, axis, route)


def normalize(values_in, gain_row):
    values = values_in.astype(jnp.float32)
    scale = lax.rsqrt(jnp.mean(values * values, axis=-1, keepdims=True) + epsilon)
    return (values * scale * gain_row.astype(jnp.float32)).astype(jnp.bfloat16)


def convolve(extended, taps):
    width = taps.shape[0]
    out_rows = extended.shape[1] - (width - 1)
    total = jnp.zeros((extended.shape[0], out_rows, extended.shape[2]), jnp.float32)
    for offset in range(width):
        total = total + taps[offset].astype(jnp.float32) * extended[:, offset : offset + out_rows]
    return total


def local(tokens, norm_gains, weight_outer, weight_inner, weight_value, conv_taps, weight_output):
    layers = conv_taps.shape[0]
    history = conv_taps.shape[1] - 1
    sequences, rows, width = tokens.shape
    channels = weight_outer.shape[2]
    weight_in = jnp.concatenate([weight_outer, weight_inner, weight_value], axis=2)
    current = tokens.reshape(sequences * rows, width)
    result = None
    for layer in range(layers):
        joined, whole = gather_all([(weight_in[layer], "sp", 0), (current, "tp", 1)], 2 * layer)
        normed = normalize(whole, norm_gains[layer])
        gates = jnp.dot(normed, joined, preferred_element_type=jnp.float32).astype(jnp.bfloat16)
        outer, inner, value = (
            gates[:, i * channels : (i + 1) * channels].reshape(sequences, rows, channels)
            for i in range(3)
        )
        gated = inner.astype(jnp.float32) * value.astype(jnp.float32)
        earlier = from_behind(gated[:, rows - history :], "sp", 1)
        extended = jnp.concatenate([earlier, gated], axis=1)
        conved = convolve(extended, conv_taps[layer])
        mixer = (outer.astype(jnp.float32) * conved).astype(jnp.bfloat16)
        flat_mixer = mixer.reshape(sequences * rows, channels)
        weight_down, full_mix = gather_all(
            [(weight_output[layer], "sp", 0), (flat_mixer, "tp", 1)], 2 * layer + 1
        )
        result = jnp.dot(full_mix, weight_down, preferred_element_type=jnp.float32)
        current = result.astype(jnp.bfloat16)
    return result.reshape(sequences, rows, width)


def solution(mesh):
    placed = (
        P(None, "sp", "tp"),
        P(),
        P(None, "sp", "tp"),
        P(None, "sp", "tp"),
        P(None, "sp", "tp"),
        P(None, None, "tp"),
        P(None, "sp", "tp"),
    )
    return jax.shard_map(
        local, mesh=mesh, in_specs=placed, out_specs=P(None, "sp", "tp"), check_vma=False
    )
```

```python
import functools

import jax
import jax.numpy as jnp
from jax import lax
from jax.experimental import pallas as pl
from jax.experimental.pallas import tpu as pltpu
from jax.sharding import PartitionSpec as P

epsilon = 1e-06


class Gather:
    def __init__(self, axis, size, dim, shard, whole, sems):
        self.axis, self.dim, self.shard, self.whole = axis, dim, shard, whole
        self.pair = 2 if size % 2 == 0 else 1
        self.length = size // self.pair
        me = lax.axis_index(axis)
        self.spot, self.side = me // self.pair, me % self.pair
        self.line_recv, self.pair_recv, self.right, self.left, self.across, self.own = sems

    def place(self, spot, side):
        extent = self.shard.shape[self.dim]
        start = pl.multiple_of((spot * self.pair + side) * extent, extent)
        cut = pl.ds(start, extent)
        return self.whole.at[cut, :] if self.dim == 0 else self.whole.at[:, cut]

    def remote(self, kind, owner, own=False):
        slot = self.place(owner, self.side)
        send, recv, target = {
            "right": (self.right, self.line_recv, (self.spot + 1) * self.pair + self.side),
            "left": (self.left, self.line_recv, (self.spot - 1) * self.pair + self.side),
            "across": (self.across, self.pair_recv, self.spot * self.pair + 1 - self.side),
        }[kind]
        return pltpu.make_async_remote_copy(
            src_ref=self.shard if own else slot,
            dst_ref=slot,
            send_sem=send.at[owner],
            recv_sem=recv.at[owner],
            device_id={self.axis: target},
        )

    def arrived(self, side, recv, owner):
        slot = self.place(owner, side)
        pltpu.make_async_remote_copy(
            src_ref=slot,
            dst_ref=slot,
            send_sem=self.across.at[owner],
            recv_sem=recv.at[owner],
            device_id={self.axis: self.spot * self.pair + self.side},
        ).wait_recv()

    def spread(self, owner, go_right, go_left, own=False):
        if go_right:
            @pl.when(self.spot < self.length - 1)
            def _():
                self.remote("right", owner, own).start()

        if go_left:
            @pl.when(self.spot > 0)
            def _():
                self.remote("left", owner, own).start()

        if self.pair == 2:
            self.remote("across", owner, own).start()

    def local(self):
        return pltpu.make_async_copy(self.shard, self.place(self.spot, self.side), self.own)

    def start(self):
        self.spread(self.spot, True, True, own=True)
        self.local().start()

    def step(self, distance):
        @pl.when(self.spot >= distance)
        def _():
            self.arrived(self.side, self.line_recv, self.spot - distance)
            self.spread(self.spot - distance, True, False)

        @pl.when(self.spot + distance < self.length)
        def _():
            self.arrived(self.side, self.line_recv, self.spot + distance)
            self.spread(self.spot + distance, False, True)

    def steps(self):
        return [functools.partial(self.step, distance) for distance in range(1, self.length)]

    def complete(self):
        self.local().wait()
        if self.pair == 2:
            for owner in range(self.length):
                self.arrived(1 - self.side, self.pair_recv, owner)

    def drain(self):
        for owner in range(self.length):
            if self.pair == 2:
                self.remote("across", owner).wait_send()

            @pl.when(jnp.logical_and(self.spot >= owner, self.spot < self.length - 1))
            def _(owner=owner):
                self.remote("right", owner).wait_send()

            @pl.when(jnp.logical_and(self.spot <= owner, self.spot > 0))
            def _(owner=owner):
                self.remote("left", owner).wait_send()


def greet(gathers):
    barrier = pltpu.get_barrier_semaphore()
    expected = jnp.int32(0)
    for g in gathers:
        for step in (-1, 1):
            there = jnp.logical_and(g.spot + step >= 0, g.spot + step < g.length)
            expected = expected + there.astype(jnp.int32)

            @pl.when(there)
            def _(g=g, step=step):
                target = (g.spot + step) * g.pair + g.side
                pl.semaphore_signal(barrier, inc=1, device_id={g.axis: target})

        if g.pair == 2:
            expected = expected + 1
            target = g.spot * g.pair + 1 - g.side
            pl.semaphore_signal(barrier, inc=1, device_id={g.axis: target})
    pl.semaphore_wait(barrier, expected)


def alternate(first, second):
    for i in range(max(len(first), len(second))):
        for actions in (first, second):
            if i < len(actions):
                actions[i]()


def sems_of(size, times=1):
    length = size // 2 if size % 2 == 0 else size
    return ([pltpu.SemaphoreType.DMA((length,))] * 5 + [pltpu.SemaphoreType.DMA]) * times


def cut_up(axis, size, pieces, shard, whole, sems):
    rows = shard.shape[0] // pieces
    return [
        Gather(axis, size, 1, shard.at[pl.ds(i * rows, rows)], whole.at[pl.ds(i * rows, rows)], sems[6 * i : 6 * i + 6])
        for i in range(pieces)
    ]


def gather_kernel(sizes, pieces, weight, acts, weight_out, acts_out, *sems):
    weights = Gather("sp", sizes[0], 0, weight, weight_out, sems[:6])
    chunks = cut_up("tp", sizes[1], pieces, acts, acts_out, sems[6:])
    greet([weights, chunks[0]])
    weights.start()
    for chunk in chunks:
        chunk.start()
    alternate([act for chunk in chunks for act in chunk.steps()], weights.steps())
    for each in chunks + [weights]:
        each.complete()
        each.drain()


def boundary_kernel(sizes, pieces, down, weight, mixer, weight_out, acts_out, down_all, mix_all, acts, *sems):
    downs = Gather("sp", sizes[0], 0, down, down_all, sems[:6])
    weights = Gather("sp", sizes[0], 0, weight, weight_out, sems[6:12])
    mixes = cut_up("tp", sizes[1], pieces, mixer, mix_all, sems[12 : 12 + 6 * pieces])
    chunks = cut_up("tp", sizes[1], pieces, acts, acts_out, sems[12 + 6 * pieces :])
    rows = mixer.shape[0] // pieces
    greet([downs, mixes[0]])
    downs.start()
    for mix in mixes:
        mix.start()
    for act in downs.steps():
        act()
    weights.start()
    downs.complete()
    for i in range(pieces):
        for act in mixes[i].steps():
            act()
        mixes[i].complete()
        cut = pl.ds(i * rows, rows)
        acts[cut, :] = jnp.dot(
            mix_all[cut, :], down_all[...], preferred_element_type=jnp.float32
        ).astype(acts.dtype)
        chunks[i].start()
    alternate([act for chunk in chunks for act in chunk.steps()], weights.steps())
    for each in chunks + [weights]:
        each.complete()
    for each in [downs] + mixes + chunks + [weights]:
        each.drain()


def grown(array, dim, size):
    shape = list(array.shape)
    shape[dim] *= size
    return jax.ShapeDtypeStruct(tuple(shape), array.dtype)


def gather_both(weight, acts, pieces, number):
    sizes = lax.axis_size("sp"), lax.axis_size("tp")
    return pl.pallas_call(
        functools.partial(gather_kernel, sizes, pieces),
        out_shape=(grown(weight, 0, sizes[0]), grown(acts, 1, sizes[1])),
        in_specs=[pl.BlockSpec(memory_space=pltpu.VMEM)] * 2,
        out_specs=(pl.BlockSpec(memory_space=pl.ANY),) * 2,
        scratch_shapes=sems_of(sizes[0]) + sems_of(sizes[1], pieces),
        compiler_params=pltpu.CompilerParams(collective_id=number, has_side_effects=True),
    )(weight, acts)


def cross_boundary(down, weight, mixer, pieces, number):
    sizes = lax.axis_size("sp"), lax.axis_size("tp")
    acts = jax.ShapeDtypeStruct((mixer.shape[0], down.shape[1]), mixer.dtype)
    down_all, mix_all = grown(down, 0, sizes[0]), grown(mixer, 1, sizes[1])
    return pl.pallas_call(
        functools.partial(boundary_kernel, sizes, pieces),
        out_shape=(grown(weight, 0, sizes[0]), grown(acts, 1, sizes[1])),
        in_specs=[pl.BlockSpec(memory_space=pltpu.VMEM)] * 3,
        out_specs=(pl.BlockSpec(memory_space=pl.ANY),) * 2,
        scratch_shapes=[pltpu.VMEM(a.shape, a.dtype) for a in (down_all, mix_all, acts)]
        + sems_of(sizes[0], 2)
        + sems_of(sizes[1], 2 * pieces),
        compiler_params=pltpu.CompilerParams(collective_id=number, has_side_effects=True),
    )(down, weight, mixer)


def from_behind(block, axis, distance):
    devices = range(lax.axis_size(axis))
    route = [(i - distance, i) for i in devices if i - distance in devices]
    return lax.ppermute(block, axis, route)


def normalize(values_in, gain_row):
    values = values_in.astype(jnp.float32)
    scale = lax.rsqrt(jnp.mean(values * values, axis=-1, keepdims=True) + epsilon)
    return (values * scale * gain_row.astype(jnp.float32)).astype(jnp.bfloat16)


def convolve(extended, taps):
    width = taps.shape[0]
    out_rows = extended.shape[1] - (width - 1)
    total = jnp.zeros((extended.shape[0], out_rows, extended.shape[2]), jnp.float32)
    for offset in range(width):
        total = total + taps[offset].astype(jnp.float32) * extended[:, offset : offset + out_rows]
    return total


def local(tokens, norm_gains, weight_outer, weight_inner, weight_value, conv_taps, weight_output):
    layers = conv_taps.shape[0]
    history = conv_taps.shape[1] - 1
    sequences, rows, width = tokens.shape
    channels = weight_outer.shape[2]
    weight_in = jnp.concatenate([weight_outer, weight_inner, weight_value], axis=2)
    joined, whole = gather_both(
        weight_in[0], tokens.reshape(sequences * rows, width), sequences, 0
    )
    for layer in range(layers):
        normed = normalize(whole, norm_gains[layer])
        gates = jnp.dot(normed, joined, preferred_element_type=jnp.float32).astype(jnp.bfloat16)
        outer, inner, value = (
            gates[:, i * channels : (i + 1) * channels].reshape(sequences, rows, channels)
            for i in range(3)
        )
        gated = inner.astype(jnp.float32) * value.astype(jnp.float32)
        earlier = from_behind(gated[:, rows - history :], "sp", 1)
        extended = jnp.concatenate([earlier, gated], axis=1)
        conved = convolve(extended, conv_taps[layer])
        mixer = (outer.astype(jnp.float32) * conved).astype(jnp.bfloat16)
        mixer = mixer.reshape(sequences * rows, channels)
        if layer < layers - 1:
            joined, whole = cross_boundary(
                weight_output[layer], weight_in[layer + 1], mixer, sequences, layer + 1
            )
    down, full_mix = gather_both(weight_output[layers - 1], mixer, sequences, layers)
    result = jnp.dot(full_mix, down, preferred_element_type=jnp.float32)
    return result.reshape(sequences, rows, width)


def solution(mesh):
    placed = (
        P(None, "sp", "tp"),
        P(),
        P(None, "sp", "tp"),
        P(None, "sp", "tp"),
        P(None, "sp", "tp"),
        P(None, None, "tp"),
        P(None, "sp", "tp"),
    )
    return jax.shard_map(
        local, mesh=mesh, in_specs=placed, out_specs=P(None, "sp", "tp"), check_vma=False
    )
```

```python
import functools

import jax
import jax.numpy as jnp
from jax import lax
from jax.experimental import pallas as pl
from jax.experimental.pallas import tpu as pltpu
from jax.sharding import PartitionSpec as P

epsilon = 1e-06


class Gather:
    def __init__(self, axis, size, dim, shard, whole, sems):
        self.axis, self.dim, self.shard, self.whole = axis, dim, shard, whole
        self.pair = 2 if size % 2 == 0 else 1
        self.length = size // self.pair
        me = lax.axis_index(axis)
        self.spot, self.side = me // self.pair, me % self.pair
        self.line_recv, self.pair_recv, self.right, self.left, self.across, self.own = sems

    def place(self, spot, side):
        extent = self.shard.shape[self.dim]
        start = pl.multiple_of((spot * self.pair + side) * extent, extent)
        cut = pl.ds(start, extent)
        return self.whole.at[cut, :] if self.dim == 0 else self.whole.at[:, cut]

    def remote(self, kind, owner, own=False):
        slot = self.place(owner, self.side)
        send, recv, target = {
            "right": (self.right, self.line_recv, (self.spot + 1) * self.pair + self.side),
            "left": (self.left, self.line_recv, (self.spot - 1) * self.pair + self.side),
            "across": (self.across, self.pair_recv, self.spot * self.pair + 1 - self.side),
        }[kind]
        return pltpu.make_async_remote_copy(
            src_ref=self.shard if own else slot,
            dst_ref=slot,
            send_sem=send.at[owner],
            recv_sem=recv.at[owner],
            device_id={self.axis: target},
        )

    def arrived(self, side, recv, owner):
        slot = self.place(owner, side)
        pltpu.make_async_remote_copy(
            src_ref=slot,
            dst_ref=slot,
            send_sem=self.across.at[owner],
            recv_sem=recv.at[owner],
            device_id={self.axis: self.spot * self.pair + self.side},
        ).wait_recv()

    def spread(self, owner, go_right, go_left, own=False):
        if go_right:
            @pl.when(self.spot < self.length - 1)
            def _():
                self.remote("right", owner, own).start()

        if go_left:
            @pl.when(self.spot > 0)
            def _():
                self.remote("left", owner, own).start()

        if self.pair == 2:
            self.remote("across", owner, own).start()

    def local(self):
        return pltpu.make_async_copy(self.shard, self.place(self.spot, self.side), self.own)

    def start(self):
        self.spread(self.spot, True, True, own=True)
        self.local().start()

    def step(self, distance):
        @pl.when(self.spot >= distance)
        def _():
            self.arrived(self.side, self.line_recv, self.spot - distance)
            self.spread(self.spot - distance, True, False)

        @pl.when(self.spot + distance < self.length)
        def _():
            self.arrived(self.side, self.line_recv, self.spot + distance)
            self.spread(self.spot + distance, False, True)

    def steps(self):
        return [functools.partial(self.step, distance) for distance in range(1, self.length)]

    def complete(self):
        self.local().wait()
        if self.pair == 2:
            for owner in range(self.length):
                self.arrived(1 - self.side, self.pair_recv, owner)

    def drain(self):
        for owner in range(self.length):
            if self.pair == 2:
                self.remote("across", owner).wait_send()

            @pl.when(jnp.logical_and(self.spot >= owner, self.spot < self.length - 1))
            def _(owner=owner):
                self.remote("right", owner).wait_send()

            @pl.when(jnp.logical_and(self.spot <= owner, self.spot > 0))
            def _(owner=owner):
                self.remote("left", owner).wait_send()


def greet(gathers):
    barrier = pltpu.get_barrier_semaphore()
    expected = jnp.int32(0)
    for g in gathers:
        for step in (-1, 1):
            there = jnp.logical_and(g.spot + step >= 0, g.spot + step < g.length)
            expected = expected + there.astype(jnp.int32)

            @pl.when(there)
            def _(g=g, step=step):
                target = (g.spot + step) * g.pair + g.side
                pl.semaphore_signal(barrier, inc=1, device_id={g.axis: target})

        if g.pair == 2:
            expected = expected + 1
            target = g.spot * g.pair + 1 - g.side
            pl.semaphore_signal(barrier, inc=1, device_id={g.axis: target})
    pl.semaphore_wait(barrier, expected)


def alternate(first, second):
    for i in range(max(len(first), len(second))):
        for actions in (first, second):
            if i < len(actions):
                actions[i]()


def sems_of(size, times=1):
    length = size // 2 if size % 2 == 0 else size
    return ([pltpu.SemaphoreType.DMA((length,))] * 5 + [pltpu.SemaphoreType.DMA]) * times


def cut_up(axis, size, pieces, shard, whole, sems):
    rows = shard.shape[0] // pieces
    return [
        Gather(axis, size, 1, shard.at[pl.ds(i * rows, rows)], whole.at[pl.ds(i * rows, rows)], sems[6 * i : 6 * i + 6])
        for i in range(pieces)
    ]


def gather_kernel(sizes, pieces, weight, acts, weight_out, acts_out, *sems):
    weights = Gather("sp", sizes[0], 0, weight, weight_out, sems[:6])
    chunks = cut_up("tp", sizes[1], pieces, acts, acts_out, sems[6:])
    greet([weights, chunks[0]])
    weights.start()
    for chunk in chunks:
        chunk.start()
    alternate([act for chunk in chunks for act in chunk.steps()], weights.steps())
    for each in chunks + [weights]:
        each.complete()
        each.drain()


def project(chunks, weights, gain, acts_all, weight_all, normed, gates):
    rows = chunks[0].shard.shape[0]
    group = 16 if rows % 16 == 0 else rows

    def norm(i):
        chunks[i].complete()

        @pl.loop(0, rows // group)
        def _(j):
            cut = pl.ds(pl.multiple_of(i * rows + j * group, group), group)
            values = acts_all[cut, :].astype(jnp.float32)
            scale = lax.rsqrt(jnp.mean(values * values, axis=-1, keepdims=True) + epsilon)
            normed[cut, :] = (values * scale * gain[...]).astype(normed.dtype)

    def multiply(i):
        cut = pl.ds(i * rows, rows)
        gates[cut, :] = jnp.dot(
            normed[cut, :], weight_all[...], preferred_element_type=jnp.float32
        ).astype(gates.dtype)

    def take(i):
        for act in chunks[i].steps():
            act()
        norm(i)

    early = max(len(chunks) - 2, 0)
    alternate([functools.partial(take, i) for i in range(early)], weights.steps())
    weights.complete()
    for i in range(early):
        multiply(i)
    for i in range(early, len(chunks)):
        take(i)
        multiply(i)


def first_kernel(sizes, pieces, weight, acts, gain, gates, weight_all, acts_all, normed, *sems):
    weights = Gather("sp", sizes[0], 0, weight, weight_all, sems[:6])
    chunks = cut_up("tp", sizes[1], pieces, acts, acts_all, sems[6:])
    greet([weights, chunks[0]])
    weights.start()
    for chunk in chunks:
        chunk.start()
    project(chunks, weights, gain, acts_all, weight_all, normed, gates)
    for each in chunks + [weights]:
        each.drain()


def boundary_kernel(sizes, pieces, down, weight, mixer, gain, gates, weight_all, acts_all, normed, down_all, mix_all, acts, *sems):
    downs = Gather("sp", sizes[0], 0, down, down_all, sems[:6])
    weights = Gather("sp", sizes[0], 0, weight, weight_all, sems[6:12])
    mixes = cut_up("tp", sizes[1], pieces, mixer, mix_all, sems[12 : 12 + 6 * pieces])
    chunks = cut_up("tp", sizes[1], pieces, acts, acts_all, sems[12 + 6 * pieces :])
    rows = mixer.shape[0] // pieces
    greet([downs, mixes[0]])
    downs.start()
    for mix in mixes:
        mix.start()
    for act in downs.steps():
        act()
    weights.start()
    downs.complete()
    for i in range(pieces):
        for act in mixes[i].steps():
            act()
        mixes[i].complete()
        cut = pl.ds(i * rows, rows)
        acts[cut, :] = jnp.dot(
            mix_all[cut, :], down_all[...], preferred_element_type=jnp.float32
        ).astype(acts.dtype)
        chunks[i].start()
    project(chunks, weights, gain, acts_all, weight_all, normed, gates)
    for each in [downs] + mixes + chunks + [weights]:
        each.drain()


def grown(array, dim, size):
    shape = list(array.shape)
    shape[dim] *= size
    return jax.ShapeDtypeStruct(tuple(shape), array.dtype)


def gather_both(weight, acts, pieces, number):
    sizes = lax.axis_size("sp"), lax.axis_size("tp")
    return pl.pallas_call(
        functools.partial(gather_kernel, sizes, pieces),
        out_shape=(grown(weight, 0, sizes[0]), grown(acts, 1, sizes[1])),
        in_specs=[pl.BlockSpec(memory_space=pltpu.VMEM)] * 2,
        out_specs=(pl.BlockSpec(memory_space=pl.ANY),) * 2,
        scratch_shapes=sems_of(sizes[0]) + sems_of(sizes[1], pieces),
        compiler_params=pltpu.CompilerParams(collective_id=number, has_side_effects=True),
    )(weight, acts)


def begin(weight, acts, gain, pieces, number):
    sizes = lax.axis_size("sp"), lax.axis_size("tp")
    weight_all, acts_all = grown(weight, 0, sizes[0]), grown(acts, 1, sizes[1])
    return pl.pallas_call(
        functools.partial(first_kernel, sizes, pieces),
        out_shape=jax.ShapeDtypeStruct((acts.shape[0], weight.shape[1]), acts.dtype),
        in_specs=[pl.BlockSpec(memory_space=pltpu.VMEM)] * 3,
        out_specs=pl.BlockSpec(memory_space=pltpu.VMEM),
        scratch_shapes=[pltpu.VMEM(a.shape, a.dtype) for a in (weight_all, acts_all, acts_all)]
        + sems_of(sizes[0])
        + sems_of(sizes[1], pieces),
        compiler_params=pltpu.CompilerParams(collective_id=number, has_side_effects=True),
    )(weight, acts, gain)


def cross_boundary(down, weight, mixer, gain, pieces, number):
    sizes = lax.axis_size("sp"), lax.axis_size("tp")
    acts = jax.ShapeDtypeStruct((mixer.shape[0], down.shape[1]), mixer.dtype)
    down_all, mix_all = grown(down, 0, sizes[0]), grown(mixer, 1, sizes[1])
    weight_all, acts_all = grown(weight, 0, sizes[0]), grown(acts, 1, sizes[1])
    held = weight_all, acts_all, acts_all, down_all, mix_all, acts
    return pl.pallas_call(
        functools.partial(boundary_kernel, sizes, pieces),
        out_shape=jax.ShapeDtypeStruct((mixer.shape[0], weight.shape[1]), mixer.dtype),
        in_specs=[pl.BlockSpec(memory_space=pltpu.VMEM)] * 4,
        out_specs=pl.BlockSpec(memory_space=pltpu.VMEM),
        scratch_shapes=[pltpu.VMEM(a.shape, a.dtype) for a in held]
        + sems_of(sizes[0], 2)
        + sems_of(sizes[1], 2 * pieces),
        compiler_params=pltpu.CompilerParams(collective_id=number, has_side_effects=True),
    )(down, weight, mixer, gain)


def from_behind(block, axis, distance):
    devices = range(lax.axis_size(axis))
    route = [(i - distance, i) for i in devices if i - distance in devices]
    return lax.ppermute(block, axis, route)


def convolve(extended, taps):
    width = taps.shape[0]
    out_rows = extended.shape[1] - (width - 1)
    total = jnp.zeros((extended.shape[0], out_rows, extended.shape[2]), jnp.float32)
    for offset in range(width):
        total = total + taps[offset].astype(jnp.float32) * extended[:, offset : offset + out_rows]
    return total


def local(tokens, norm_gains, weight_outer, weight_inner, weight_value, conv_taps, weight_output):
    layers = conv_taps.shape[0]
    history = conv_taps.shape[1] - 1
    sequences, rows, width = tokens.shape
    channels = weight_outer.shape[2]
    weight_in = jnp.concatenate([weight_outer, weight_inner, weight_value], axis=2)
    tokens = tokens.reshape(sequences * rows, width)
    gates = begin(weight_in[0], tokens, norm_gains[:1], sequences, 0)
    for layer in range(layers):
        outer, inner, value = (
            gates[:, i * channels : (i + 1) * channels].reshape(sequences, rows, channels)
            for i in range(3)
        )
        gated = inner.astype(jnp.float32) * value.astype(jnp.float32)
        earlier = from_behind(gated[:, rows - history :], "sp", 1)
        extended = jnp.concatenate([earlier, gated], axis=1)
        conved = convolve(extended, conv_taps[layer])
        mixer = (outer.astype(jnp.float32) * conved).astype(jnp.bfloat16)
        mixer = mixer.reshape(sequences * rows, channels)
        if layer < layers - 1:
            following = layer + 1
            gain = norm_gains[following : following + 1]
            gates = cross_boundary(
                weight_output[layer], weight_in[following], mixer, gain, sequences, following
            )
    down, full_mix = gather_both(weight_output[layers - 1], mixer, sequences, layers)
    result = jnp.dot(full_mix, down, preferred_element_type=jnp.float32)
    return result.reshape(sequences, rows, width)


def solution(mesh):
    placed = (
        P(None, "sp", "tp"),
        P(),
        P(None, "sp", "tp"),
        P(None, "sp", "tp"),
        P(None, "sp", "tp"),
        P(None, None, "tp"),
        P(None, "sp", "tp"),
    )
    return jax.shard_map(
        local, mesh=mesh, in_specs=placed, out_specs=P(None, "sp", "tp"), check_vma=False
    )
```
